32 devices in a mesh: sp: 4 (over y, x), tp: 8 (over z, core).
Axes of the slice: x: 2, y: 2, z: 4, core: 2. Of those that a mesh axis runs over, the one named last changes fastest.
Arguments:
- target: bfloat16 [512, 2048], P('sp'), may hold values from -6 to 6
- source: bfloat16 [1536, 2048], P('sp'), may hold values from -6 to 6
- cotangent: bfloat16 [512, 2048], P('sp'), may hold values from -192 to 192
- target_gain: float32 [2048], replicated, may hold values from 0.1 to 1.9
- source_gain: float32 [2048], replicated, may hold values from 0.1 to 1.9
- w_query: bfloat16 [2048, 4096], P(None, 'tp'), may hold values from -0.125 to 0.125
- w_key: bfloat16 [2048, 128], replicated, may hold values from -0.125 to 0.125
- w_value: bfloat16 [2048, 128], replicated, may hold values from -0.125 to 0.125
- w_out: bfloat16 [4096, 2048], P('tp'), may hold values from -0.09375 to 0.09375
Outputs:
- grad_target: bfloat16 [512, 2048], P(('sp', 'tp'))
- grad_source: bfloat16 [1536, 2048], P(('sp', 'tp'))
- grad_out_w: bfloat16 [4096, 2048], P('tp', 'sp')
The draws below stay inside these ranges and needn't reach their ends.
All inputs are finite; a program needn't handle non-finite values.
Results may differ from the reference program's by a relative error of at most 0.025.
Values may be sent and summed in bfloat16 or wider, within the bound.
A program may use at most 64 MiB of HBM per device.

```python
import jax
import jax.numpy as jnp
from jax import lax

D = 2048
HEADS = 32
HEAD = 128
TARGET = 512
SOURCE = 1536


def steps_of(own_key, dims, shards, low, largest):
    level = 1.0
    for dim, shards_of in shards:
        draws = jax.random.uniform(jax.random.fold_in(jax.random.fold_in(own_key, 6), dim), (shards_of,), jnp.float32, low / len(shards), largest / len(shards))
        level = level * jnp.repeat(jnp.exp(draws), dims[dim] // shards_of).reshape((-1,) + (1,) * (len(dims) - 1 - dim))
    return level


def bell_draw(own_key, extent, spread, bound, split=(), kind=jnp.bfloat16):
    result = spread * jax.random.normal(own_key, extent, jnp.float32)
    if split:
        result = result * steps_of(own_key, extent, split, -0.22, 0.18)
    return jnp.clip(result, -bound, bound).astype(kind)


def setup_inputs(seed: int = 0) -> dict:
    key_of = jax.random.split(jax.random.key(seed), 10)
    return {
        "target": bell_draw(key_of[0], (TARGET, D), 1.0, 6.0, ((0, 4),)),
        "source": bell_draw(key_of[1], (SOURCE, D), 1.0, 6.0, ((0, 4),)),
        "cotangent": bell_draw(key_of[2], (TARGET, D), 32.0, 192.0, ((0, 4),)),
        "target_gain": jnp.clip(1.0 + 0.18 * jax.random.normal(key_of[3], (D,), jnp.float32), 0.1, 1.9),
        "source_gain": jnp.clip(1.0 + 0.18 * jax.random.normal(key_of[4], (D,), jnp.float32), 0.1, 1.9),
        "w_query": bell_draw(key_of[5], (D, HEADS * HEAD), D ** -0.5, 0.125, ((1, 8),)),
        "w_key": bell_draw(key_of[6], (D, HEAD), D ** -0.5, 0.125),
        "w_value": bell_draw(key_of[7], (D, HEAD), D ** -0.5, 0.125),
        "w_out": bell_draw(key_of[8], (HEADS * HEAD, D), (HEADS * HEAD) ** -0.5, 0.09375, ((0, 8),)),
    }


NORM_EPS = 1e-06

def normed(row_block, gain_vec):
    rows_wide = row_block.astype(jnp.float32)
    inv_rms = lax.rsqrt(lax.optimization_barrier(jnp.mean(rows_wide * rows_wide, axis=1, keepdims=True)) + NORM_EPS)
    return (rows_wide * inv_rms * gain_vec).astype(jnp.bfloat16)

def norm_back(row_block, gain_vec, upstream):
    rows_wide = row_block.astype(jnp.float32)
    inv_rms = lax.rsqrt(lax.optimization_barrier(jnp.mean(rows_wide * rows_wide, axis=1, keepdims=True)) + NORM_EPS)
    unit_rows = rows_wide * inv_rms
    pulled = upstream * gain_vec
    return inv_rms * (pulled - unit_rows * lax.optimization_barrier(jnp.mean(pulled * unit_rows, axis=1, keepdims=True)))

def reference(target, source, cotangent, target_gain, source_gain, w_query, w_key, w_value, w_out):
    inv_root = HEAD ** (-0.5)
    normed_target = normed(target, target_gain)
    query_rows = jnp.dot(normed_target, w_query, preferred_element_type=jnp.float32).astype(jnp.bfloat16)
    normed_source = normed(source, source_gain)
    key_rows = jnp.dot(normed_source, w_key, preferred_element_type=jnp.float32).astype(jnp.bfloat16)
    value_rows = jnp.dot(normed_source, w_value, preferred_element_type=jnp.float32).astype(jnp.bfloat16)
    grad_attn = jnp.dot(cotangent, w_out.T, preferred_element_type=jnp.float32).astype(jnp.bfloat16)
    query_heads = query_rows.reshape(TARGET, HEADS, HEAD).transpose(1, 0, 2)
    grad_heads = grad_attn.reshape(TARGET, HEADS, HEAD).transpose(1, 0, 2)

    def one_head(carried, head_pair):
        key_sum, value_sum = carried
        query_one, grad_one = head_pair
        scores = jnp.dot(query_one, key_rows.T, preferred_element_type=jnp.float32) * inv_root
        exponent = jnp.exp(scores)
        row_total = lax.optimization_barrier(jnp.sum(exponent, axis=1))
        weights = exponent.astype(jnp.bfloat16)
        attended = (jnp.dot(weights, value_rows, preferred_element_type=jnp.float32) / row_total[:, None]).astype(jnp.bfloat16)
        prob_grad = jnp.dot(grad_one, value_rows.T, preferred_element_type=jnp.float32)
        delta_row = lax.optimization_barrier(jnp.sum(attended.astype(jnp.float32) * grad_one.astype(jnp.float32), axis=1))
        tilted = (exponent * prob_grad).astype(jnp.bfloat16)
        tilted_sum = jnp.dot(tilted, key_rows, preferred_element_type=jnp.float32)
        weight_sum = jnp.dot(weights, key_rows, preferred_element_type=jnp.float32)
        grad_query = ((tilted_sum - delta_row[:, None] * weight_sum) / row_total[:, None] * inv_root).astype(jnp.bfloat16)
        prob_rows = exponent / row_total[:, None]
        score_grad = (prob_rows * (prob_grad - delta_row[:, None])).astype(jnp.bfloat16)
        key_grad = jnp.dot(score_grad.T, query_one, preferred_element_type=jnp.float32) * inv_root
        value_grad = jnp.dot(prob_rows.astype(jnp.bfloat16).T, grad_one, preferred_element_type=jnp.float32)
        return ((key_sum + key_grad, value_sum + value_grad), (attended, grad_query))
    empty_keys = jnp.zeros((SOURCE, HEAD), jnp.float32)
    sums, stacked = lax.scan(one_head, (empty_keys, empty_keys), (query_heads, grad_heads))
    key_grad, value_grad = sums
    attended_heads, query_grad_heads = stacked
    attended_rows = attended_heads.transpose(1, 0, 2).reshape(TARGET, HEADS * HEAD)
    query_grad_rows = query_grad_heads.transpose(1, 0, 2).reshape(TARGET, HEADS * HEAD)
    pulled_source = jnp.dot(key_grad.astype(jnp.bfloat16), w_key.T, preferred_element_type=jnp.float32)
    pulled_source = pulled_source + jnp.dot(value_grad.astype(jnp.bfloat16), w_value.T, preferred_element_type=jnp.float32)
    grad_source = norm_back(source, source_gain, pulled_source).astype(jnp.bfloat16)
    pulled_target = jnp.dot(query_grad_rows, w_query.T, preferred_element_type=jnp.float32)
    grad_target = norm_back(target, target_gain, pulled_target).astype(jnp.bfloat16)
    grad_out_w = jnp.dot(attended_rows.T, cotangent, preferred_element_type=jnp.float32).astype(jnp.bfloat16)
    return (grad_target, grad_source, grad_out_w)
```

```python
import functools
import math

import jax
import jax.numpy as jnp
from jax import lax
from jax.experimental import pallas as pl
from jax.experimental.pallas import tpu as pltpu
from jax.sharding import PartitionSpec as P

HEAD = 128
NORM_EPS = 1e-06
CORES = 2
F32 = jnp.float32
BF16 = jnp.bfloat16
MESH = pl.DeviceIdType.MESH
NN = (((1,), (0,)), ((), ()))
NT = (((1,), (1,)), ((), ()))
TN = (((0,), (0,)), ((), ()))


def dot(a, b, dims=NN):
    return lax.dot_general(a, b, dims, preferred_element_type=F32)


def inv_rms_of(wide):
    return lax.rsqrt(jnp.mean(wide * wide, axis=1, keepdims=True) + NORM_EPS)


def gained(src, gain, dst, rows):
    D = src.shape[1]
    step = 256
    squares = None
    for at in range(0, D, step):
        columns = slice(at, at + step)
        wide = src[rows, columns].astype(F32)
        dst[rows, columns] = (wide * gain[:, columns]).astype(BF16)
        part = wide * wide
        part = sum(part[:, i:i + 128] for i in range(0, step, 128))
        squares = part if squares is None else squares + part
    return lax.rsqrt(jnp.sum(squares, axis=1, keepdims=True) * (1.0 / D) + NORM_EPS)


def norm_back(wide, gain, upstream):
    inv = inv_rms_of(wide)
    unit = wide * inv
    pulled = upstream * gain
    return inv * (pulled - unit * jnp.mean(pulled * unit, axis=1, keepdims=True))


def own_rows(ref, place, rows):
    if rows % 16 == 0:
        return ref[pl.ds(pl.multiple_of(place * rows, 16), rows), :].astype(F32)
    padded = -(-rows // 16) * 16
    line = lax.broadcasted_iota(jnp.int32, (padded, ref.shape[0]), 0) + place * rows
    column = lax.broadcasted_iota(jnp.int32, (padded, ref.shape[0]), 1)
    pick = jnp.where(line == column, 1.0, 0.0).astype(BF16)
    return dot(pick, ref[...])[:rows]


def kernel(
    S, T,
    target_h, source_h, cot_h, tgain_h, sgain_h, wq_h, wk_h, wv_h, wo_h,
    gt_ref, gs_ref, go_ref,
    target, source, cot, tgain, sgain, wq, wkv, wo, normed, kv, cotb, att, e_buf, pg_buf,
    kvg, kvg_in, red, red_in, red2, fin_in, pt, pt_in, ptr, ptr_in, stage, wide_stage,
    load_sem, send, recv,
):
    Z = T // CORES
    me, t = lax.axis_index("sp"), lax.axis_index("tp")
    c, z = lax.rem(t, CORES), lax.div(t, CORES)
    sibling = {"sp": me, "tp": z * CORES + (1 - c)}
    TR, D = target.shape
    SG = source.shape[0]
    QW = wq.shape[1]
    H = QW // HEAD
    half = SG // 2
    thalf = TR // 2
    W = D // S
    SR, RR = SG // T, TR // T
    inv_root = HEAD ** (-0.5)
    parts = next(n for n in (3, 2, 1) if half % (16 * n) == 0)
    chunk = half // parts

    X = math.isqrt(S) if math.isqrt(S) ** 2 == S else S
    Y = S // X
    steps = sorted(
        ((i // X, i % X) for i in range(S)), key=lambda yx: ((yx[0] > 0) + (yx[1] > 0), yx)
    )
    near = [d for d in range(1, S) if 0 in steps[d]]
    far = [d for d in range(1, S) if 0 not in steps[d]]

    def sp_place(d, way=1):
        dy, dx = steps[d]
        y = lax.rem(lax.div(me, X) + (dy if way > 0 else Y - dy), Y)
        x = lax.rem(lax.rem(me, X) + (dx if way > 0 else X - dx), X)
        return y * X + x

    def sp_peer(d, way=1):
        return {"sp": sp_place(d, way), "tp": t}

    def z_peer(d):
        return {"sp": me, "tp": lax.rem(z + d, Z) * CORES + c}

    sends = []

    def put(src, dst, who):
        lane = len(sends)
        copy = pltpu.make_async_remote_copy(
            src_ref=src, dst_ref=dst, send_sem=send.at[lane], recv_sem=recv.at[lane],
            device_id=who, device_id_type=MESH,
        )
        copy.start()
        sends.append(copy)
        return copy

    def own_half(i):
        return pl.ds(pl.multiple_of(c * half + i * chunk, chunk), chunk)

    others = pl.ds(pl.multiple_of((1 - c) * half, half), half)
    pairs = [
        (sgain_h, sgain), (source_h.at[own_half(0)], source.at[own_half(0)]),
        (wk_h, wkv.at[:, :HEAD]), (wv_h, wkv.at[:, HEAD:]),
        (tgain_h, tgain), (target_h, target), (wq_h, wq), (cot_h, cot), (wo_h, wo),
        (source_h.at[others], source.at[others]),
    ] + [(source_h.at[own_half(i)], source.at[own_half(i)]) for i in range(1, parts)]
    loads = [pltpu.make_async_copy(a, b, load_sem.at[i]) for i, (a, b) in enumerate(pairs)]
    for i in (0, 1, 2, 3, *range(10, 9 + parts)):
        loads[i].start()

    barrier = pltpu.get_barrier_semaphore()
    friends = [sibling] + [sp_peer(d) for d in range(1, S)] + [z_peer(d) for d in range(1, Z)]
    for who in friends:
        pl.semaphore_signal(barrier, inc=1, device_id=who, device_id_type=MESH)

    kv_put = {d: [] for d in range(1, S)}
    for i in range(parts):
        if i == 0:
            loads[0].wait()
            loads[1].wait()
            for j in (5, 4, 7, 6, 8, 9):
                loads[j].start()
        else:
            loads[9 + i].wait()
        inv = gained(source, sgain, normed, own_half(i))
        if i == 0:
            loads[2].wait()
            loads[3].wait()
        rows = pl.ds(i * chunk, chunk)
        kv[0, c, rows, :] = (dot(normed[own_half(i), :], wkv[...]) * inv).astype(BF16)
        if i == 0:
            pl.semaphore_wait(barrier, len(friends))
        for d in far + near:
            kv_put[d].append(put(kv.at[0, c, rows], kv.at[d, c, rows], sp_peer(d)))
    kv_twin = put(kv.at[0, c], kv.at[0, c], sibling)
    loads[5].wait()
    loads[4].wait()
    inv = gained(target, tgain, normed, slice(0, TR))
    loads[6].wait()
    query = dot(normed[:TR, :], wq[...]) * inv
    loads[7].wait()
    loads[8].wait()
    grad = dot(cot[...], wo[...], NT)
    split = [slice(h * HEAD, (h + 1) * HEAD) for h in range(H)]
    q_rows = jnp.concatenate([query[:, h] for h in split], axis=0).astype(BF16)
    g_rows = jnp.concatenate([grad[:, h] for h in split], axis=0).astype(BF16)
    q_cols = jnp.concatenate([query[:, h].T for h in split], axis=1).astype(BF16)
    g_cols = jnp.concatenate([grad[:, h].T for h in split], axis=1).astype(BF16)

    def forward(blocks):
        both = jnp.concatenate([kv[d, part] for d, part in blocks], axis=0)
        k, v = both[:, :HEAD], both[:, HEAD:]
        e = jnp.exp2(dot(k, q_cols) * (inv_root * math.log2(math.e)))
        prob_grad = dot(v, g_cols)
        for i, (d, part) in enumerate(blocks):
            e_buf[d, part] = e[i * half:(i + 1) * half]
            pg_buf[d, part] = prob_grad[i * half:(i + 1) * half]
        tilted = (e * prob_grad).astype(BF16)
        return jnp.sum(e, axis=0, keepdims=True), dot(both, e.astype(BF16), TN), dot(k, tilted, TN)

    def more(state, blocks):
        return tuple(a + b for a, b in zip(state, forward(blocks)))

    kv_fwd = {}

    def hand_on(places):
        for d in places:
            for copy in kv_put[d]:
                copy.wait_recv()
            kv_fwd[d] = put(kv.at[d, c], kv.at[d, c], sibling)

    loads[9].wait()
    kv_twin.wait_recv()
    state = forward([(0, c), (0, 1 - c)])
    hand_on(near + far)
    cot_put = [None]
    for d in range(1, S):
        columns = pl.ds(pl.multiple_of(sp_place(d) * W, 128), W)
        rows = pl.ds(pl.multiple_of(c * thalf, thalf), thalf)
        cot_put.append(put(cot.at[rows, columns], cotb.at[d, c], sp_peer(d)))

    state = more(state, [(d, c) for d in near + far])
    for d in near + far:
        kv_fwd[d].wait_recv()
    state = more(state, [(d, 1 - c) for d in near + far])
    total, weighted, tilted_sum = state
    inv_total = 1.0 / total
    att_t = (weighted[HEAD:] * inv_total).astype(BF16)
    att[0] = att_t
    top, bottom = pl.ds(0, HEAD // 2), pl.ds(HEAD // 2, HEAD // 2)
    att_put = {d: [] for d in range(1, S)}
    for d in near:
        att_put[d].append(put(att.at[0, top], att.at[d, top], sp_peer(d)))
    delta = jnp.sum(att_t.astype(F32) * g_cols.astype(F32), axis=0, keepdims=True)

    def spread(d, grads):
        if SR % 8:
            stage[...] = grads
        for place in range(T):
            rows = slice(place * SR, (place + 1) * SR)
            block = stage[rows, :] if SR % 8 else grads[rows]
            kvg[place % CORES, d, place // CORES] = block.astype(BF16)

    kvg_put = {}
    red_put = {}
    pieces = [1, 2, 3, 0] if Z == 4 else [None]

    def backward(d):
        p = e_buf[d].reshape(SG, -1) * inv_total
        score_grad = (p * (pg_buf[d].reshape(SG, -1) - delta)).astype(BF16)
        k_grad = dot(score_grad, q_rows) * inv_root
        v_grad = dot(p.astype(BF16), g_rows)
        spread(d, jnp.concatenate([k_grad, v_grad], axis=1))
        kvg_put[d] = put(kvg.at[1 - c, d], kvg_in.at[d], sibling)

    def settle(d):
        kvg_put[d].wait_recv()
        red[d] = (kvg[c, d].astype(F32) + kvg_in[d].astype(F32)).astype(BF16)
        if d:
            red_put[d] = []
            for j in pieces:
                at = pl.ds(0, Z) if j is None else pl.ds(lax.rem(z + j, Z), 1)
                red_put[d].append(put(red.at[d, at], red_in.at[d, at], sp_peer(d, -1)))

    order = list(range(S - 1, -1, -1))
    backward(order[0])
    gq_t = (tilted_sum - delta * weighted[:HEAD]) * (inv_total * inv_root)
    gq = jnp.concatenate([gq_t[:, h * TR:(h + 1) * TR].T for h in range(H)], axis=1).astype(BF16)
    bands = [slice(i * (D // 2), (i + 1) * (D // 2)) for i in range(2)]
    pt_put = []
    for i, band in enumerate(bands):
        pulled = dot(gq, wq[band, :], NT)
        if RR % 8:
            wide_stage[...] = pulled
        for place in range(T):
            rows = slice(place * RR, (place + 1) * RR)
            block = wide_stage[rows, :] if RR % 8 else pulled[rows]
            pt[place % CORES, i, place // CORES] = block.astype(BF16)
        pt_put.append(put(pt.at[1 - c, i], pt_in.at[i], sibling))
    settle(order[0])
    for d in near:
        att_put[d].append(put(att.at[0, bottom], att.at[d, bottom], sp_peer(d)))
    backward(order[1])
    z_order = sorted(range(1, Z), key=lambda d: (abs(Z // 2 - d), d))
    ptr_put = {d: [] for d in z_order}
    for i in range(2):
        pt_put[i].wait_recv()
        ptr[i] = (pt[c, i].astype(F32) + pt_in[i].astype(F32)).astype(BF16)
        for d in z_order:
            ptr_put[d].append(put(ptr.at[i, lax.rem(z + d, Z)], ptr_in.at[i, d], z_peer(d)))
    for before, d in zip(order[1:], order[2:]):
        backward(d)
        settle(before)
    settle(0)
    for d in far:
        att_put[d].append(put(att.at[0], att.at[d], sp_peer(d)))
    cot_fwd = [None]
    for d in range(1, S):
        cot_put[d].wait_recv()
        cot_fwd.append(put(cotb.at[d, c], cotb.at[d, c], sibling))

    fin_put = {}
    for n, j in enumerate(pieces):
        at = pl.ds(0, Z) if j is None else pl.ds(lax.rem(z + j, Z), 1)
        summed = red[0, at].astype(F32)
        for d in range(1, S):
            red_put[d][n].wait_recv()
            summed = summed + red_in[d, at].astype(F32)
        red2[at] = summed.astype(BF16)
        for d in z_order if j is None else [j] if j else []:
            fin_put[d] = put(red2.at[lax.rem(z + d, Z)], fin_in.at[d], z_peer(d))

    ups = []
    for i in range(2):
        up = ptr[i, z].astype(F32)
        for d in z_order:
            ptr_put[d][i].wait_recv()
            up = up + ptr_in[i, d].astype(F32)
        ups.append(up)
    up = jnp.concatenate(ups, axis=1)
    gt_ref[...] = norm_back(own_rows(target, t, RR), tgain[...], up).astype(BF16)

    def go_part(places):
        rows, lefts = [], []
        for d in places:
            if d:
                for copy in att_put[d]:
                    copy.wait_recv()
                cot_fwd[d].wait_recv()
                rows.append(jnp.concatenate([cotb[d, 0], cotb[d, 1]], axis=0))
            else:
                rows.append(cot[:, pl.ds(pl.multiple_of(me * W, 128), W)])
            lefts.append(att[d])
        right = jnp.concatenate(rows, axis=0)
        return [
            dot(jnp.concatenate([a[:, h * TR:(h + 1) * TR] for a in lefts], axis=1), right)
            for h in range(H)
        ]

    first, second = go_part(range(S // 2)), go_part(range(S // 2, S))
    for h in range(H):
        go_ref[h * HEAD:(h + 1) * HEAD, :] = (first[h] + second[h]).astype(BF16)

    last = red2[z].astype(F32)
    for d in z_order:
        fin_put[d].wait_recv()
        last = last + fin_in[d].astype(F32)
    up = dot(last.astype(BF16), wkv[...], NT)
    gs_ref[...] = norm_back(own_rows(source, t, SR), sgain[...], up).astype(BF16)
    for copy in sends:
        copy.wait_send()


def on_device(S, T, target, source, cotangent, target_gain, source_gain, w_query, w_key, w_value, w_out):
    TR, D = target.shape
    SG = source.shape[0]
    QW = w_query.shape[1]
    R = QW // HEAD * TR
    Z = T // CORES
    SR, RR, W = SG // T, TR // T, D // S
    N = 3 * (S - 1) + 3 * (S - 1) + 2 * (S - 1) + (S - 1) + S + 4 * (S - 1) + 3 * Z + 5
    hbm = pl.BlockSpec(memory_space=pltpu.HBM)
    vmem = pl.BlockSpec(memory_space=pltpu.VMEM)
    V = pltpu.VMEM
    results = pl.pallas_call(
        functools.partial(kernel, S, T),
        out_shape=(
            V((RR, D), BF16), V((SR, D), BF16), V((QW, W), BF16),
        ),
        in_specs=[hbm] * 9,
        out_specs=(vmem, vmem, vmem),
        scratch_shapes=[
            V((TR, D), BF16), V((SG, D), BF16), V((TR, D), BF16), V((1, D), F32), V((1, D), F32),
            V((D, QW), BF16), V((D, 2 * HEAD), BF16), V((QW, D), BF16),
            V((max(SG, TR), D), BF16),
            V((S, 2, SG // 2, 2 * HEAD), BF16), V((S, 2, TR // 2, W), BF16),
            V((S, HEAD, R), BF16), V((S, 2, SG // 2, R), F32), V((S, 2, SG // 2, R), F32),
            V((CORES, S, Z, SR, 2 * HEAD), BF16), V((S, Z, SR, 2 * HEAD), BF16),
            V((S, Z, SR, 2 * HEAD), BF16), V((S, Z, SR, 2 * HEAD), BF16),
            V((Z, SR, 2 * HEAD), BF16), V((Z, SR, 2 * HEAD), BF16),
            V((CORES, 2, Z, RR, D // 2), BF16), V((2, Z, RR, D // 2), BF16),
            V((2, Z, RR, D // 2), BF16), V((2, Z, RR, D // 2), BF16),
            V((SG, 2 * HEAD), F32), V((TR, D // 2) if RR % 8 else (8, 128), F32),
            pltpu.SemaphoreType.DMA((12,)),
            pltpu.SemaphoreType.DMA((N,)),
            pltpu.SemaphoreType.DMA((N,)),
        ],
        compiler_params=pltpu.CompilerParams(
            collective_id=0, has_side_effects=True, vmem_limit_bytes=60 * 1024 * 1024
        ),
        name="attn_back",
    )(
        target, source, cotangent, target_gain.reshape(1, D), source_gain.reshape(1, D),
        w_query, w_key, w_value, w_out,
    )
    return pl.pallas_call(
        put_out,
        out_shape=tuple(jax.ShapeDtypeStruct(r.shape, r.dtype) for r in results),
        in_specs=[vmem, vmem, vmem],
        out_specs=(hbm, hbm, hbm),
        scratch_shapes=[pltpu.SemaphoreType.DMA((3,))],
        compiler_params=pltpu.CompilerParams(vmem_limit_bytes=60 * 1024 * 1024),
        name="put_out",
    )(*[pltpu.with_memory_space_constraint(r, pltpu.VMEM) for r in results])


def put_out(a, b, c, a_out, b_out, c_out, sem):
    outs = [
        pltpu.make_async_copy(x, y, sem.at[i])
        for i, (x, y) in enumerate(((a, a_out), (b, b_out), (c, c_out)))
    ]
    for copy in outs:
        copy.start()
    for copy in outs:
        copy.wait()


def solution(mesh):
    in_specs = (
        P("sp", None), P("sp", None), P("sp", None), P(), P(),
        P(None, "tp"), P(), P(), P("tp", None),
    )
    out_specs = (P(("sp", "tp"), None), P(("sp", "tp"), None), P("tp", "sp"))
    return jax.shard_map(
        functools.partial(on_device, mesh.shape["sp"], mesh.shape["tp"]),
        mesh=mesh, in_specs=in_specs, out_specs=out_specs, check_vma=False,
    )
```

```python
import functools
import math

import jax
import jax.numpy as jnp
from jax import lax
from jax.experimental import pallas as pl
from jax.experimental.pallas import tpu as pltpu
from jax.sharding import PartitionSpec as P

HEAD = 128
NORM_EPS = 1e-06
CORES = 2
F32 = jnp.float32
BF16 = jnp.bfloat16
MESH = pl.DeviceIdType.MESH
NN = (((1,), (0,)), ((), ()))
NT = (((1,), (1,)), ((), ()))
TN = (((0,), (0,)), ((), ()))


def dot(a, b, dims=NN):
    return lax.dot_general(a, b, dims, preferred_element_type=F32)


def inv_rms_of(wide):
    return lax.rsqrt(jnp.mean(wide * wide, axis=1, keepdims=True) + NORM_EPS)


def gained(src, gain, dst, rows):
    D = src.shape[1]
    step = 256
    squares = None
    for at in range(0, D, step):
        columns = slice(at, at + step)
        wide = src[rows, columns].astype(F32)
        dst[rows, columns] = (wide * gain[:, columns]).astype(BF16)
        part = wide * wide
        part = sum(part[:, i:i + 128] for i in range(0, step, 128))
        squares = part if squares is None else squares + part
    return lax.rsqrt(jnp.sum(squares, axis=1, keepdims=True) * (1.0 / D) + NORM_EPS)


def unit_of(wide):
    inv = inv_rms_of(wide)
    return inv, wide * inv


def norm_back(inv, unit, gain, upstream):
    pulled = upstream * gain
    return inv * (pulled - unit * jnp.mean(pulled * unit, axis=1, keepdims=True))


def own_rows(ref, place, rows):
    if rows % 16 == 0:
        return ref[pl.ds(pl.multiple_of(place * rows, 16), rows), :].astype(F32)
    padded = -(-rows // 16) * 16
    line = lax.broadcasted_iota(jnp.int32, (padded, ref.shape[0]), 0) + place * rows
    column = lax.broadcasted_iota(jnp.int32, (padded, ref.shape[0]), 1)
    pick = jnp.where(line == column, 1.0, 0.0).astype(BF16)
    return dot(pick, ref[...])[:rows]


def kernel(
    S, T,
    target_h, source_h, cot_h, tgain_h, sgain_h, wq_h, wk_h, wv_h, wo_h,
    gt_ref, gs_ref, go_ref,
    target, source, cot, tgain, sgain, wq, wkv, wo, normed, kv, cotb, att, e_buf, pg_buf,
    kvg, kvg_in, red, red_in, red2, fin_in, pt, pt_in, ptr, ptr_in, pt_out, stage, wide_stage,
    load_sem, send, recv,
):
    Z = T // CORES
    me, t = lax.axis_index("sp"), lax.axis_index("tp")
    c, z = lax.rem(t, CORES), lax.div(t, CORES)
    sibling = {"sp": me, "tp": z * CORES + (1 - c)}
    TR, D = target.shape
    SG = source.shape[0]
    QW = wq.shape[1]
    H = QW // HEAD
    half = SG // 2
    thalf = TR // 2
    W = D // S
    SR, RR = SG // T, TR // T
    inv_root = HEAD ** (-0.5)
    parts = next(n for n in (3, 2, 1) if half % (16 * n) == 0)
    chunk = half // parts

    X = math.isqrt(S) if math.isqrt(S) ** 2 == S else S
    Y = S // X
    steps = sorted(
        ((i // X, i % X) for i in range(S)), key=lambda yx: ((yx[0] > 0) + (yx[1] > 0), yx)
    )
    near = [d for d in range(1, S) if 0 in steps[d]]
    far = [d for d in range(1, S) if 0 not in steps[d]]

    def sp_place(d, way=1):
        dy, dx = steps[d]
        y = lax.rem(lax.div(me, X) + (dy if way > 0 else Y - dy), Y)
        x = lax.rem(lax.rem(me, X) + (dx if way > 0 else X - dx), X)
        return y * X + x

    def sp_peer(d, way=1):
        return {"sp": sp_place(d, way), "tp": t}

    def z_peer(d):
        return {"sp": me, "tp": lax.rem(z + d, Z) * CORES + c}

    twin_z = z + 1 - 2 * lax.rem(z, 2)
    twin = {"sp": me, "tp": twin_z * CORES + c}
    rest = pl.ds(1, S - 1)

    sends, lanes = [], []

    def put(src, dst, who):
        lane = len(lanes)
        lanes.append(lane)
        copy = pltpu.make_async_remote_copy(
            src_ref=src, dst_ref=dst, send_sem=send.at[lane], recv_sem=recv.at[lane],
            device_id=who, device_id_type=MESH,
        )
        copy.start()
        sends.append(copy)
        return copy

    def gone(copies):
        for copy in copies:
            copy.wait_send()
            sends[:] = [other for other in sends if other is not copy]

    def own_half(i):
        return pl.ds(pl.multiple_of(c * half + i * chunk, chunk), chunk)

    others = pl.ds(pl.multiple_of((1 - c) * half, half), half)
    pairs = [
        (sgain_h, sgain), (source_h.at[own_half(0)], source.at[own_half(0)]),
        (wk_h, wkv.at[:, :HEAD]), (wv_h, wkv.at[:, HEAD:]),
        (tgain_h, tgain), (target_h, target), (wq_h, wq), (cot_h, cot), (wo_h, wo),
        (source_h.at[others], source.at[others]),
    ] + [(source_h.at[own_half(i)], source.at[own_half(i)]) for i in range(1, parts)]
    loads = [pltpu.make_async_copy(a, b, load_sem.at[i]) for i, (a, b) in enumerate(pairs)]
    for i in (0, 1, 2, 3):
        loads[i].start()

    barrier = pltpu.get_barrier_semaphore()
    friends = [sibling] + [sp_peer(d) for d in range(1, S)] + [z_peer(d) for d in range(1, Z)]
    for who in friends:
        pl.semaphore_signal(barrier, inc=1, device_id=who, device_id_type=MESH)

    kv_put = {d: [] for d in range(1, S)}
    for i in range(parts):
        if i == 0:
            loads[0].wait()
            loads[1].wait()
            for j in (*range(10, 9 + parts), 5, 4, 7, 6, 8, 9):
                loads[j].start()
        else:
            loads[9 + i].wait()
        inv = gained(source, sgain, normed, own_half(i))
        if i == 0:
            loads[2].wait()
            loads[3].wait()
        rows = pl.ds(i * chunk, chunk)
        kv[0, c, rows, :] = (dot(normed[own_half(i), :], wkv[...]) * inv).astype(BF16)
        if i == 0:
            pl.semaphore_wait(barrier, len(friends))
        for d in far + near:
            kv_put[d].append(put(kv.at[0, c, rows], kv.at[d, c, rows], sp_peer(d)))
    kv_twin = put(kv.at[0, c], kv.at[0, c], sibling)
    loads[5].wait()
    loads[4].wait()
    inv = gained(target, tgain, normed, slice(0, TR))
    loads[6].wait()
    query = dot(normed[:TR, :], wq[...]) * inv
    loads[7].wait()
    loads[8].wait()
    grad = dot(cot[...], wo[...], NT)
    split = [slice(h * HEAD, (h + 1) * HEAD) for h in range(H)]
    split_rows = [slice(h * TR, (h + 1) * TR) for h in range(H)]
    q_rows = jnp.concatenate([query[:, h] for h in split], axis=0).astype(BF16)
    g_rows = jnp.concatenate([grad[:, h] for h in split], axis=0).astype(BF16)
    q_cols = jnp.concatenate([query[:, h].T for h in split], axis=1).astype(BF16)
    g_cols = jnp.concatenate([grad[:, h].T for h in split], axis=1).astype(BF16)

    def forward(blocks):
        both = jnp.concatenate([kv[block] for block in blocks], axis=0)
        k, v = both[:, :HEAD], both[:, HEAD:]
        e = jnp.exp2(dot(k, q_cols) * (inv_root * math.log2(math.e)))
        prob_grad = dot(v, g_cols)
        at = 0
        for block in blocks:
            count = block[2].size
            e_buf[block] = e[at:at + count]
            pg_buf[block] = prob_grad[at:at + count]
            at += count
        tilted = (e * prob_grad).astype(BF16)
        return jnp.sum(e, axis=0, keepdims=True), dot(both, e.astype(BF16), TN), dot(k, tilted, TN)

    def more(state, blocks):
        return tuple(a + b for a, b in zip(state, forward(blocks)))

    loads[9].wait()
    kv_twin.wait_recv()
    chunks = [pl.ds(i * chunk, chunk) for i in range(parts)]
    state = forward([(0, part, rows) for part in (c, 1 - c) for rows in chunks])
    kv_fwd = []
    cot_put = []
    held = []
    for i, rows in enumerate(chunks):
        for d in near + far:
            kv_put[d][i].wait_recv()
            kv_fwd.append(put(kv.at[d, c, rows], kv.at[d, c, rows], sibling))
        if i:
            for copy in kv_fwd[(i - 1) * (S - 1):i * (S - 1)]:
                copy.wait_recv()
        state = more(state, [(d, c, rows) for d in near + far] + held)
        held = [(d, 1 - c, rows) for d in near + far]
        if i == 0:
            gone([copy for d in kv_put for copy in kv_put[d]])
            lines = pl.ds(pl.multiple_of(c * thalf, thalf), thalf)
            for d in range(1, S):
                columns = pl.ds(pl.multiple_of(sp_place(d) * W, 128), W)
                cot_put.append(put(cot.at[lines, columns], cotb.at[d, c], sp_peer(d)))
    for copy in kv_fwd[-(S - 1):]:
        copy.wait_recv()
    state = more(state, held)
    total, weighted, tilted_sum = state
    inv_total = 1.0 / total
    att_t = (weighted[HEAD:] * inv_total).astype(BF16)
    att[0] = att_t
    top, bottom = pl.ds(0, HEAD * 5 // 8), pl.ds(HEAD * 5 // 8, HEAD * 3 // 8)
    att_put = {d: [] for d in range(1, S)}
    for d in near:
        att_put[d].append(put(att.at[0, top], att.at[d, top], sp_peer(d)))
    delta = jnp.sum(att_t.astype(F32) * g_cols.astype(F32), axis=0, keepdims=True)

    def spread(d, grads):
        if SR % 8:
            stage[...] = grads
        for place in range(T):
            rows = slice(place * SR, (place + 1) * SR)
            block = stage[rows, :] if SR % 8 else grads[rows]
            kvg[place % CORES, d, place // CORES] = block.astype(BF16)

    kvg_put = {}
    red_put = {}
    pieces = [1, 2, 3, 0] if Z == 4 else [None]

    def backward(d):
        p = e_buf[d].reshape(SG, -1) * inv_total
        score_grad = (p * (pg_buf[d].reshape(SG, -1) - delta)).astype(BF16)
        k_grad = dot(score_grad, q_rows) * inv_root
        v_grad = dot(p.astype(BF16), g_rows)
        spread(d, jnp.concatenate([k_grad, v_grad], axis=1))
        kvg_put[d] = put(kvg.at[1 - c, d], kvg_in.at[d], sibling)

    def settle(d):
        kvg_put[d].wait_recv()
        red[d] = (kvg[c, d].astype(F32) + kvg_in[d].astype(F32)).astype(BF16)
        if d:
            red_put[d] = []
            for j in pieces:
                at = pl.ds(0, Z) if j is None else pl.ds(lax.rem(z + j, Z), 1)
                red_put[d].append(put(red.at[d, at], red_in.at[d, at], sp_peer(d, -1)))

    order = list(range(S - 1, -1, -1))
    z_order = sorted(range(1, Z), key=lambda d: (abs(Z // 2 - d), d))
    pt_put = []
    ptr_put = [[], []]
    relayed = [0] if Z == 4 else []

    def pull(i):
        pulled = dot(gq, wq[bands[i], :], NT)
        if RR % 8:
            wide_stage[...] = pulled
        for place in range(T):
            rows = slice(place * RR, (place + 1) * RR)
            block = wide_stage[rows, :] if RR % 8 else pulled[rows]
            pt[place % CORES, i, place // CORES] = block.astype(BF16)
        pt_put.append(put(pt.at[1 - c, i], pt_in.at[i], sibling))

    def send_pulled(i):
        pt_put[i].wait_recv()
        ptr[i] = (pt[c, i].astype(F32) + pt_in[i].astype(F32)).astype(BF16)
        if i in relayed:
            ptr_put[i].append(put(ptr.at[i, lax.rem(twin_z + 2, Z)], ptr_in.at[i, 0], twin))
            ptr_put[i].append(put(ptr.at[i, twin_z], ptr_in.at[i, 1], twin))
        else:
            for d in z_order:
                ptr_put[i].append(put(ptr.at[i, lax.rem(z + d, Z)], ptr_in.at[i, d], z_peer(d)))

    def relay_pulled(i):
        ptr_put[i].pop(0).wait_recv()
        across = lax.rem(z + 2, Z)
        pt_out[...] = (ptr[i, across].astype(F32) + ptr_in[i, 0].astype(F32)).astype(BF16)
        ptr_put[i].append(put(pt_out, ptr_in.at[i, 2], z_peer(2)))

    backward(order[0])
    gq_t = (tilted_sum - delta * weighted[:HEAD]) * (inv_total * inv_root)
    gq = jnp.concatenate([gq_t[:, h].T for h in split_rows], axis=1).astype(BF16)
    bands = [slice(i * (D // 2), (i + 1) * (D // 2)) for i in range(2)]
    pull(0)
    backward(order[1])
    settle(order[0])
    pull(1)
    for copy in cot_put:
        copy.wait_recv()
    for i, d in enumerate(order[2:]):
        backward(d)
        if i < 2:
            send_pulled(i)
        settle(order[i + 1])
    for i in range(S - 2, 2):
        send_pulled(i)
    settle(0)
    for i in relayed:
        relay_pulled(i)
    for d in near:
        att_put[d][0].wait_recv()
    for d in far:
        dy, dx = steps[d]
        side = steps.index((0, dx))
        att_put[d].append(put(att.at[0, bottom], att.at[d, bottom], sp_peer(d)))
        att_put[d].append(put(att.at[side, top], att.at[d, top], sp_peer(steps.index((dy, 0)))))
    for d in near:
        att_put[d].append(put(att.at[0, bottom], att.at[d, bottom], sp_peer(d)))
    cot_fwd = put(cotb.at[rest, c], cotb.at[rest, c], sibling)

    target_unit = unit_of(own_rows(target, t, RR))
    source_unit = unit_of(own_rows(source, t, SR))
    fin_put = {}
    for n, j in enumerate(pieces):
        at = pl.ds(0, Z) if j is None else pl.ds(lax.rem(z + j, Z), 1)
        summed = red[0, at].astype(F32)
        for d in range(1, S):
            red_put[d][n].wait_recv()
            summed = summed + red_in[d, at].astype(F32)
        red2[at] = summed.astype(BF16)
        for d in z_order if j is None else [j] if j else []:
            fin_put[d] = put(red2.at[lax.rem(z + d, Z)], fin_in.at[d], z_peer(d))

    ups = []
    for i in range(2):
        for copy in ptr_put[i]:
            copy.wait_recv()
        up = ptr[i, z].astype(F32)
        for d in (1, 2) if i in relayed else z_order:
            up = up + ptr_in[i, d].astype(F32)
        ups.append(up)
    up = jnp.concatenate(ups, axis=1)
    gt_ref[...] = norm_back(*target_unit, tgain[...], up).astype(BF16)

    def go_part(places):
        rows, lefts = [], []
        for d in places:
            if d:
                for copy in att_put[d][1 if d in near else 0:]:
                    copy.wait_recv()
                rows.append(cotb[d].reshape(TR, W))
            else:
                rows.append(cot[:, pl.ds(pl.multiple_of(me * W, 128), W)])
            lefts.append(att[d])
        right = jnp.concatenate(rows, axis=0)
        return [
            dot(jnp.concatenate([a[:, h * TR:(h + 1) * TR] for a in lefts], axis=1), right)
            for h in range(H)
        ]

    cot_fwd.wait_recv()
    first = go_part(range(S // 2))
    last = red2[z].astype(F32)
    for d in z_order:
        fin_put[d].wait_recv()
        last = last + fin_in[d].astype(F32)
    up = dot(last.astype(BF16), wkv[...], NT)
    gs_ref[...] = norm_back(*source_unit, sgain[...], up).astype(BF16)
    second = go_part(range(S // 2, S))
    for h in range(H):
        go_ref[h * HEAD:(h + 1) * HEAD, :] = (first[h] + second[h]).astype(BF16)
    for copy in sends:
        copy.wait_send()


def on_device(S, T, target, source, cotangent, target_gain, source_gain, w_query, w_key, w_value, w_out):
    TR, D = target.shape
    SG = source.shape[0]
    QW = w_query.shape[1]
    R = QW // HEAD * TR
    Z = T // CORES
    SR, RR, W = SG // T, TR // T, D // S
    N = 3 * (S - 1) + 3 * (S - 1) + 2 * (S - 1) + (S - 1) + S + 4 * (S - 1) + 3 * Z + 5
    hbm = pl.BlockSpec(memory_space=pltpu.HBM)
    vmem = pl.BlockSpec(memory_space=pltpu.VMEM)
    V = pltpu.VMEM
    results = pl.pallas_call(
        functools.partial(kernel, S, T),
        out_shape=(
            V((RR, D), BF16), V((SR, D), BF16), V((QW, W), BF16),
        ),
        in_specs=[hbm] * 9,
        out_specs=(vmem, vmem, vmem),
        scratch_shapes=[
            V((TR, D), BF16), V((SG, D), BF16), V((TR, D), BF16), V((1, D), F32), V((1, D), F32),
            V((D, QW), BF16), V((D, 2 * HEAD), BF16), V((QW, D), BF16),
            V((max(SG, TR), D), BF16),
            V((S, 2, SG // 2, 2 * HEAD), BF16), V((S, 2, TR // 2, W), BF16),
            V((S, HEAD, R), BF16), V((S, 2, SG // 2, R), F32), V((S, 2, SG // 2, R), F32),
            V((CORES, S, Z, SR, 2 * HEAD), BF16), V((S, Z, SR, 2 * HEAD), BF16),
            V((S, Z, SR, 2 * HEAD), BF16), V((S, Z, SR, 2 * HEAD), BF16),
            V((Z, SR, 2 * HEAD), BF16), V((Z, SR, 2 * HEAD), BF16),
            V((CORES, 2, Z, RR, D // 2), BF16), V((2, Z, RR, D // 2), BF16),
            V((2, Z, RR, D // 2), BF16), V((2, Z, RR, D // 2), BF16), V((RR, D // 2), BF16),
            V((SG, 2 * HEAD), F32), V((TR, D // 2) if RR % 8 else (8, 128), F32),
            pltpu.SemaphoreType.DMA((12,)),
            pltpu.SemaphoreType.DMA((N,)),
            pltpu.SemaphoreType.DMA((N,)),
        ],
        compiler_params=pltpu.CompilerParams(
            collective_id=0, has_side_effects=True, vmem_limit_bytes=60 * 1024 * 1024
        ),
        name="attn_back",
    )(
        target, source, cotangent, target_gain.reshape(1, D), source_gain.reshape(1, D),
        w_query, w_key, w_value, w_out,
    )
    return pl.pallas_call(
        put_out,
        out_shape=tuple(jax.ShapeDtypeStruct(r.shape, r.dtype) for r in results),
        in_specs=[vmem, vmem, vmem],
        out_specs=(hbm, hbm, hbm),
        scratch_shapes=[pltpu.SemaphoreType.DMA((3,))],
        compiler_params=pltpu.CompilerParams(vmem_limit_bytes=60 * 1024 * 1024),
        name="put_out",
    )(*[pltpu.with_memory_space_constraint(r, pltpu.VMEM) for r in results])


def put_out(a, b, c, a_out, b_out, c_out, sem):
    outs = [
        pltpu.make_async_copy(x, y, sem.at[i])
        for i, (x, y) in enumerate(((a, a_out), (b, b_out), (c, c_out)))
    ]
    for copy in outs:
        copy.start()
    for copy in outs:
        copy.wait()


def solution(mesh):
    in_specs = (
        P("sp", None), P("sp", None), P("sp", None), P(), P(),
        P(None, "tp"), P(), P(), P("tp", None),
    )
    out_specs = (P(("sp", "tp"), None), P(("sp", "tp"), None), P("tp", "sp"))
    return jax.shard_map(
        functools.partial(on_device, mesh.shape["sp"], mesh.shape["tp"]),
        mesh=mesh, in_specs=in_specs, out_specs=out_specs, check_vma=False,
    )
```

```python
import functools
import math

import jax
import jax.numpy as jnp
from jax import lax
from jax.experimental import pallas as pl
from jax.experimental.pallas import tpu as pltpu
from jax.sharding import PartitionSpec as P

HEAD = 128
NORM_EPS = 1e-06
CORES = 2
F32 = jnp.float32
BF16 = jnp.bfloat16
MESH = pl.DeviceIdType.MESH
NN = (((1,), (0,)), ((), ()))
NT = (((1,), (1,)), ((), ()))
TN = (((0,), (0,)), ((), ()))


def dot(a, b, dims=NN):
    return lax.dot_general(a, b, dims, preferred_element_type=F32)


def inv_rms_of(wide):
    return lax.rsqrt(jnp.mean(wide * wide, axis=1, keepdims=True) + NORM_EPS)


def gained(src, gain, dst, rows):
    D = src.shape[1]
    step = 256
    squares = None
    for at in range(0, D, step):
        columns = slice(at, at + step)
        wide = src[rows, columns].astype(F32)
        dst[rows, columns] = (wide * gain[:, columns]).astype(BF16)
        part = wide * wide
        part = sum(part[:, i:i + 128] for i in range(0, step, 128))
        squares = part if squares is None else squares + part
    return lax.rsqrt(jnp.sum(squares, axis=1, keepdims=True) * (1.0 / D) + NORM_EPS)


def unit_of(wide):
    inv = inv_rms_of(wide)
    return inv, wide * inv


def norm_back(inv, unit, gain, upstream):
    pulled = upstream * gain
    return inv * (pulled - unit * jnp.mean(pulled * unit, axis=1, keepdims=True))


def own_rows(ref, place, rows):
    if rows % 16 == 0:
        return ref[pl.ds(pl.multiple_of(place * rows, 16), rows), :].astype(F32)
    padded = -(-rows // 16) * 16
    line = lax.broadcasted_iota(jnp.int32, (padded, ref.shape[0]), 0) + place * rows
    column = lax.broadcasted_iota(jnp.int32, (padded, ref.shape[0]), 1)
    pick = jnp.where(line == column, 1.0, 0.0).astype(BF16)
    return dot(pick, ref[...])[:rows]


def kernel(
    S, T,
    target_h, source_h, cot_h, tgain_h, sgain_h, wq_h, wk_h, wv_h, wo_h,
    gt_ref, gs_ref, go_ref,
    target, source, cot, tgain, sgain, wq, wkv, wo, normed, kv, cotb, att, e_buf, pg_buf,
    kvg, kvg_in, red, red_in, red2, fin_in, pt, pt_in, ptr, ptr_in, pt_out, stage, wide_stage,
    load_sem, send, recv,
):
    Z = T // CORES
    me, t = lax.axis_index("sp"), lax.axis_index("tp")
    c, z = lax.rem(t, CORES), lax.div(t, CORES)
    sibling = {"sp": me, "tp": z * CORES + (1 - c)}
    TR, D = target.shape
    SG = source.shape[0]
    QW = wq.shape[1]
    H = QW // HEAD
    half = SG // 2
    thalf = TR // 2
    W = D // S
    SR, RR = SG // T, TR // T
    inv_root = HEAD ** (-0.5)
    parts = next(n for n in (3, 2, 1) if half % (16 * n) == 0)
    chunk = half // parts

    X = math.isqrt(S) if math.isqrt(S) ** 2 == S else S
    Y = S // X
    steps = sorted(
        ((i // X, i % X) for i in range(S)), key=lambda yx: ((yx[0] > 0) + (yx[1] > 0), yx)
    )
    near = [d for d in range(1, S) if 0 in steps[d]]
    far = [d for d in range(1, S) if 0 not in steps[d]]

    def sp_place(d, way=1):
        dy, dx = steps[d]
        y = lax.rem(lax.div(me, X) + (dy if way > 0 else Y - dy), Y)
        x = lax.rem(lax.rem(me, X) + (dx if way > 0 else X - dx), X)
        return y * X + x

    def sp_peer(d, way=1):
        return {"sp": sp_place(d, way), "tp": t}

    def z_peer(d):
        return {"sp": me, "tp": lax.rem(z + d, Z) * CORES + c}

    twin_z = z + 1 - 2 * lax.rem(z, 2)
    twin = {"sp": me, "tp": twin_z * CORES + c}
    rest = pl.ds(1, S - 1)

    sends, lanes = [], []

    def put(src, dst, who):
        lane = len(lanes)
        lanes.append(lane)
        copy = pltpu.make_async_remote_copy(
            src_ref=src, dst_ref=dst, send_sem=send.at[lane], recv_sem=recv.at[lane],
            device_id=who, device_id_type=MESH,
        )
        copy.start()
        sends.append(copy)
        return copy

    def gone(copies):
        for copy in copies:
            copy.wait_send()
            sends[:] = [other for other in sends if other is not copy]

    def own_half(i):
        return pl.ds(pl.multiple_of(c * half + i * chunk, chunk), chunk)

    others = pl.ds(pl.multiple_of((1 - c) * half, half), half)
    pairs = [
        (sgain_h, sgain), (source_h.at[own_half(0)], source.at[own_half(0)]),
        (wk_h, wkv.at[:, :HEAD]), (wv_h, wkv.at[:, HEAD:]),
        (tgain_h, tgain), (target_h, target), (wq_h, wq), (cot_h, cot), (wo_h, wo),
        (source_h.at[others], source.at[others]),
    ] + [(source_h.at[own_half(i)], source.at[own_half(i)]) for i in range(1, parts)]
    loads = [pltpu.make_async_copy(a, b, load_sem.at[i]) for i, (a, b) in enumerate(pairs)]
    for i in (2, 3, 1, 0):
        loads[i].start()

    barrier = pltpu.get_barrier_semaphore()
    friends = [sibling] + [sp_peer(d) for d in range(1, S)] + [z_peer(d) for d in range(1, Z)]
    for who in friends:
        pl.semaphore_signal(barrier, inc=1, device_id=who, device_id_type=MESH)

    kv_put = {d: [] for d in range(1, S)}
    for i in range(parts):
        if i == 0:
            loads[0].wait()
            loads[1].wait()
            for j in (*range(10, 9 + parts), 5, 4, 7, 6, 8, 9):
                loads[j].start()
        else:
            loads[9 + i].wait()
        inv = gained(source, sgain, normed, own_half(i))
        if i == 0:
            loads[2].wait()
            loads[3].wait()
        rows = pl.ds(i * chunk, chunk)
        kv[0, c, rows, :] = (dot(normed[own_half(i), :], wkv[...]) * inv).astype(BF16)
        if i == 0:
            pl.semaphore_wait(barrier, len(friends))
        for d in far + near:
            kv_put[d].append(put(kv.at[0, c, rows], kv.at[d, c, rows], sp_peer(d)))
    kv_twin = put(kv.at[0, c], kv.at[0, c], sibling)
    loads[5].wait()
    loads[4].wait()
    inv = gained(target, tgain, normed, slice(0, TR))
    loads[6].wait()
    query = dot(normed[:TR, :], wq[...]) * inv
    loads[7].wait()
    loads[8].wait()
    grad = dot(cot[...], wo[...], NT)
    split = [slice(h * HEAD, (h + 1) * HEAD) for h in range(H)]
    split_rows = [slice(h * TR, (h + 1) * TR) for h in range(H)]
    q_rows = jnp.concatenate([query[:, h] for h in split], axis=0).astype(BF16)
    g_rows = jnp.concatenate([grad[:, h] for h in split], axis=0).astype(BF16)
    q_cols = jnp.concatenate([query[:, h].T for h in split], axis=1).astype(BF16)
    g_cols = jnp.concatenate([grad[:, h].T for h in split], axis=1).astype(BF16)

    def forward(blocks):
        both = jnp.concatenate([kv[block] for block in blocks], axis=0)
        k, v = both[:, :HEAD], both[:, HEAD:]
        e = jnp.exp2(dot(k, q_cols) * (inv_root * math.log2(math.e)))
        prob_grad = dot(v, g_cols)
        at = 0
        for block in blocks:
            count = block[2].size
            e_buf[block] = e[at:at + count]
            pg_buf[block] = prob_grad[at:at + count]
            at += count
        tilted = (e * prob_grad).astype(BF16)
        return jnp.sum(e, axis=0, keepdims=True), dot(both, e.astype(BF16), TN), dot(k, tilted, TN)

    def more(state, blocks):
        return tuple(a + b for a, b in zip(state, forward(blocks)))

    loads[9].wait()
    kv_twin.wait_recv()
    chunks = [pl.ds(i * chunk, chunk) for i in range(parts)]
    state = forward([(0, part, rows) for part in (c, 1 - c) for rows in chunks])
    kv_fwd = []
    cot_put = []
    held = []
    for i, rows in enumerate(chunks):
        for d in near + far:
            kv_put[d][i].wait_recv()
            kv_fwd.append(put(kv.at[d, c, rows], kv.at[d, c, rows], sibling))
        if i:
            for copy in kv_fwd[(i - 1) * (S - 1):i * (S - 1)]:
                copy.wait_recv()
        state = more(state, [(d, c, rows) for d in near + far] + held)
        held = [(d, 1 - c, rows) for d in near + far]
        if i == 0:
            gone([copy for d in kv_put for copy in kv_put[d]])
            lines = pl.ds(pl.multiple_of(c * thalf, thalf), thalf)
            for d in range(1, S):
                columns = pl.ds(pl.multiple_of(sp_place(d) * W, 128), W)
                cot_put.append(put(cot.at[lines, columns], cotb.at[d, c], sp_peer(d)))
    for copy in kv_fwd[-(S - 1):]:
        copy.wait_recv()
    state = more(state, held)
    total, weighted, tilted_sum = state
    inv_total = 1.0 / total
    att_t = (weighted[HEAD:] * inv_total).astype(BF16)
    att[0] = att_t
    top, bottom = pl.ds(0, HEAD * 5 // 8), pl.ds(HEAD * 5 // 8, HEAD * 3 // 8)
    att_put = {d: [] for d in range(1, S)}
    for d in near:
        att_put[d].append(put(att.at[0, top], att.at[d, top], sp_peer(d)))
    delta = jnp.sum(att_t.astype(F32) * g_cols.astype(F32), axis=0, keepdims=True)

    def spread(d, grads):
        if SR % 8:
            stage[...] = grads
        for place in range(T):
            rows = slice(place * SR, (place + 1) * SR)
            block = stage[rows, :] if SR % 8 else grads[rows]
            kvg[place % CORES, d, place // CORES] = block.astype(BF16)

    kvg_put = {}
    red_put = {}
    pieces = [1, 2, 3, 0] if Z == 4 else [None]

    def backward(d):
        p = e_buf[d].reshape(SG, -1) * inv_total
        score_grad = (p * (pg_buf[d].reshape(SG, -1) - delta)).astype(BF16)
        k_grad = dot(score_grad, q_rows) * inv_root
        v_grad = dot(p.astype(BF16), g_rows)
        spread(d, jnp.concatenate([k_grad, v_grad], axis=1))
        kvg_put[d] = put(kvg.at[1 - c, d], kvg_in.at[d], sibling)

    def settle(d):
        kvg_put[d].wait_recv()
        red[d] = (kvg[c, d].astype(F32) + kvg_in[d].astype(F32)).astype(BF16)
        if d:
            red_put[d] = []
            for j in pieces:
                at = pl.ds(0, Z) if j is None else pl.ds(lax.rem(z + j, Z), 1)
                red_put[d].append(put(red.at[d, at], red_in.at[d, at], sp_peer(d, -1)))

    order = list(range(S - 1, -1, -1))
    z_order = sorted(range(1, Z), key=lambda d: (abs(Z // 2 - d), d))
    pt_put = []
    ptr_put = [[], []]
    relayed = [0] if Z == 4 else []

    def pull(i):
        pulled = dot(gq, wq[bands[i], :], NT)
        if RR % 8:
            wide_stage[...] = pulled
        for place in range(T):
            rows = slice(place * RR, (place + 1) * RR)
            block = wide_stage[rows, :] if RR % 8 else pulled[rows]
            pt[place % CORES, i, place // CORES] = block.astype(BF16)
        pt_put.append(put(pt.at[1 - c, i], pt_in.at[i], sibling))

    def send_pulled(i):
        pt_put[i].wait_recv()
        ptr[i] = (pt[c, i].astype(F32) + pt_in[i].astype(F32)).astype(BF16)
        if i in relayed:
            ptr_put[i].append(put(ptr.at[i, lax.rem(twin_z + 2, Z)], ptr_in.at[i, 0], twin))
            ptr_put[i].append(put(ptr.at[i, twin_z], ptr_in.at[i, 1], twin))
        else:
            for d in z_order:
                ptr_put[i].append(put(ptr.at[i, lax.rem(z + d, Z)], ptr_in.at[i, d], z_peer(d)))

    def relay_pulled(i):
        ptr_put[i].pop(0).wait_recv()
        across = lax.rem(z + 2, Z)
        pt_out[...] = (ptr[i, across].astype(F32) + ptr_in[i, 0].astype(F32)).astype(BF16)
        ptr_put[i].append(put(pt_out, ptr_in.at[i, 2], z_peer(2)))

    backward(order[0])
    gq_t = (tilted_sum - delta * weighted[:HEAD]) * (inv_total * inv_root)
    gq = jnp.concatenate([gq_t[:, h].T for h in split_rows], axis=1).astype(BF16)
    bands = [slice(i * (D // 2), (i + 1) * (D // 2)) for i in range(2)]
    pull(0)
    backward(order[1])
    settle(order[0])
    pull(1)
    for copy in cot_put:
        copy.wait_recv()
    for i, d in enumerate(order[2:]):
        backward(d)
        if i < 2:
            send_pulled(i)
        settle(order[i + 1])
    for i in range(S - 2, 2):
        send_pulled(i)
    settle(0)
    for d in far + near:
        att_put[d].append(put(att.at[0, bottom], att.at[d, bottom], sp_peer(d)))
    for i in relayed:
        relay_pulled(i)
    for d in near:
        att_put[d][0].wait_recv()
    for d in far:
        dy, dx = steps[d]
        side = steps.index((0, dx))
        att_put[d].append(put(att.at[side, top], att.at[d, top], sp_peer(steps.index((dy, 0)))))
    cot_fwd = put(cotb.at[rest, c], cotb.at[rest, c], sibling)

    target_unit = unit_of(own_rows(target, t, RR))
    source_unit = unit_of(own_rows(source, t, SR))
    fin_put = {}
    for n, j in enumerate(pieces):
        at = pl.ds(0, Z) if j is None else pl.ds(lax.rem(z + j, Z), 1)
        summed = red[0, at].astype(F32)
        for d in range(1, S):
            red_put[d][n].wait_recv()
            summed = summed + red_in[d, at].astype(F32)
        red2[at] = summed.astype(BF16)
        for d in z_order if j is None else [j] if j else []:
            fin_put[d] = put(red2.at[lax.rem(z + d, Z)], fin_in.at[d], z_peer(d))

    ups = []
    for i in range(2):
        for copy in ptr_put[i]:
            copy.wait_recv()
        up = ptr[i, z].astype(F32)
        for d in (1, 2) if i in relayed else z_order:
            up = up + ptr_in[i, d].astype(F32)
        ups.append(up)
    up = jnp.concatenate(ups, axis=1)
    gt_ref[...] = norm_back(*target_unit, tgain[...], up).astype(BF16)

    def go_part(places):
        rows, lefts = [], []
        for d in places:
            if d:
                for copy in att_put[d][1 if d in near else 0:]:
                    copy.wait_recv()
                rows.append(cotb[d].reshape(TR, W))
            else:
                rows.append(cot[:, pl.ds(pl.multiple_of(me * W, 128), W)])
            lefts.append(att[d])
        right = jnp.concatenate(rows, axis=0)
        return [
            dot(jnp.concatenate([a[:, h * TR:(h + 1) * TR] for a in lefts], axis=1), right)
            for h in range(H)
        ]

    cot_fwd.wait_recv()
    first = go_part(range(S // 2))
    last = red2[z].astype(F32)
    for d in z_order:
        fin_put[d].wait_recv()
        last = last + fin_in[d].astype(F32)
    up = dot(last.astype(BF16), wkv[...], NT)
    gs_ref[...] = norm_back(*source_unit, sgain[...], up).astype(BF16)
    second = go_part(range(S // 2, S))
    for h in range(H):
        go_ref[h * HEAD:(h + 1) * HEAD, :] = (first[h] + second[h]).astype(BF16)
    for copy in sends:
        copy.wait_send()


def on_device(S, T, target, source, cotangent, target_gain, source_gain, w_query, w_key, w_value, w_out):
    TR, D = target.shape
    SG = source.shape[0]
    QW = w_query.shape[1]
    R = QW // HEAD * TR
    Z = T // CORES
    SR, RR, W = SG // T, TR // T, D // S
    N = 3 * (S - 1) + 3 * (S - 1) + 2 * (S - 1) + (S - 1) + S + 4 * (S - 1) + 3 * Z + 5
    hbm = pl.BlockSpec(memory_space=pltpu.HBM)
    vmem = pl.BlockSpec(memory_space=pltpu.VMEM)
    V = pltpu.VMEM
    results = pl.pallas_call(
        functools.partial(kernel, S, T),
        out_shape=(
            V((RR, D), BF16), V((SR, D), BF16), V((QW, W), BF16),
        ),
        in_specs=[hbm] * 9,
        out_specs=(vmem, vmem, vmem),
        scratch_shapes=[
            V((TR, D), BF16), V((SG, D), BF16), V((TR, D), BF16), V((1, D), F32), V((1, D), F32),
            V((D, QW), BF16), V((D, 2 * HEAD), BF16), V((QW, D), BF16),
            V((max(SG, TR), D), BF16),
            V((S, 2, SG // 2, 2 * HEAD), BF16), V((S, 2, TR // 2, W), BF16),
            V((S, HEAD, R), BF16), V((S, 2, SG // 2, R), F32), V((S, 2, SG // 2, R), F32),
            V((CORES, S, Z, SR, 2 * HEAD), BF16), V((S, Z, SR, 2 * HEAD), BF16),
            V((S, Z, SR, 2 * HEAD), BF16), V((S, Z, SR, 2 * HEAD), BF16),
            V((Z, SR, 2 * HEAD), BF16), V((Z, SR, 2 * HEAD), BF16),
            V((CORES, 2, Z, RR, D // 2), BF16), V((2, Z, RR, D // 2), BF16),
            V((2, Z, RR, D // 2), BF16), V((2, Z, RR, D // 2), BF16), V((RR, D // 2), BF16),
            V((SG, 2 * HEAD), F32), V((TR, D // 2) if RR % 8 else (8, 128), F32),
            pltpu.SemaphoreType.DMA((12,)),
            pltpu.SemaphoreType.DMA((N,)),
            pltpu.SemaphoreType.DMA((N,)),
        ],
        compiler_params=pltpu.CompilerParams(
            collective_id=0, has_side_effects=True, vmem_limit_bytes=60 * 1024 * 1024
        ),
        name="attn_back",
    )(
        target, source, cotangent, target_gain.reshape(1, D), source_gain.reshape(1, D),
        w_query, w_key, w_value, w_out,
    )
    return pl.pallas_call(
        put_out,
        out_shape=tuple(jax.ShapeDtypeStruct(r.shape, r.dtype) for r in results),
        in_specs=[vmem, vmem, vmem],
        out_specs=(hbm, hbm, hbm),
        scratch_shapes=[pltpu.SemaphoreType.DMA((3,))],
        compiler_params=pltpu.CompilerParams(vmem_limit_bytes=60 * 1024 * 1024),
        name="put_out",
    )(*[pltpu.with_memory_space_constraint(r, pltpu.VMEM) for r in results])


def put_out(a, b, c, a_out, b_out, c_out, sem):
    outs = [
        pltpu.make_async_copy(x, y, sem.at[i])
        for i, (x, y) in enumerate(((a, a_out), (b, b_out), (c, c_out)))
    ]
    for copy in outs:
        copy.start()
    for copy in outs:
        copy.wait()


def solution(mesh):
    in_specs = (
        P("sp", None), P("sp", None), P("sp", None), P(), P(),
        P(None, "tp"), P(), P(), P("tp", None),
    )
    out_specs = (P(("sp", "tp"), None), P(("sp", "tp"), None), P("tp", "sp"))
    return jax.shard_map(
        functools.partial(on_device, mesh.shape["sp"], mesh.shape["tp"]),
        mesh=mesh, in_specs=in_specs, out_specs=out_specs, check_vma=False,
    )
```
